512 devices in a mesh: sp: 64 (over z, y), tp: 8 (over x, core).
Axes of the slice: x: 4, y: 8, z: 8, core: 2. Of those that a mesh axis runs over, the one named last changes fastest.
Arguments:
- skip_path_inputs: bfloat16 [8192, 2048], P('sp'), may hold values from -62 to 62
- probe_vectors: bfloat16 [8192, 1024], P('sp', 'tp'), may hold values from -6 to 6
- lookup_vectors: bfloat16 [8192, 1024], P('sp', 'tp'), may hold values from -6 to 6
- payload_vectors: bfloat16 [8192, 1024], P('sp', 'tp'), may hold values from -6 to 6
- learning_strength_preacts: float32 [2, 8192, 8], P(None, 'sp', 'tp'), may hold values from -6 to 6
- forget_preacts: float32 [2, 8192, 8], P(None, 'sp', 'tp'), may hold values from -5 to 5
- forgetting_speed_exponent: float32 [2, 8], P(None, 'tp'), may hold values from -12 to -2
- extra_forgetting_spikes: float32 [2, 8192, 8], P(None, 'sp', 'tp'), may hold values from -0.7 to 0
- sample_membership: int32 [8192], P('sp'), may hold values from 0 to 15, never falling along the last dimension, each value on 1 to 1024 neighbouring positions
- channel_group_scaling: float32 [128], replicated, may hold values from 0.1 to 1.9
- blend_exit_weights: bfloat16 [1024, 2048], P('tp'), may hold values from -0.1875 to 0.1875
- dense_block_scaling: float32 [2048], replicated, may hold values from 0.1 to 1.9
- widen_projection_weights: bfloat16 [2048, 8192], P('sp', 'tp'), may hold values from -0.125 to 0.125
- shrink_projection_weights: bfloat16 [8192, 2048], P('tp', 'sp'), may hold values from -0.0625 to 0.0625
Outputs:
- result: bfloat16 [8192, 2048], P('sp', 'tp')
The draws below stay inside these ranges and needn't reach their ends.
Inputs may be any that keep to these rules, and one draw needn't show every extreme that they name: `sample_membership`: document numbers never fall along the positions; each document holds 1 to 1024 positions.
All inputs are finite; a program needn't handle non-finite values.
Results may differ from the reference program's by a relative error of at most 0.015.
Values may be sent and summed in bfloat16 or wider, within the bound.
No kernel may reach another device: no remote copies, remote signals or barrier semaphores. Data moves between devices by JAX's collectives and lax.ppermute only.
A program may use at most 64 MiB of HBM per device.

```python
import math
import jax
import jax.numpy as jnp
import numpy as np
from jax import lax

D = 2048
HEADS = 8
HEAD = 128
FF = 8192
BLOCK = 64
TOK_DEV = 128
TOKENS = 8192
DOCS = 16
DOC_MOST = 1024
N_TP = 8


def draw_skip_path_inputs(key, part):
    pieces = jax.random.split(key, 2)
    base = jnp.clip(jax.random.normal(pieces[0], (TOKENS, D), jnp.float32), -5.0, 5.0)
    ramp = jnp.exp(math.log(3.0) * (jnp.arange(D, dtype=jnp.float32) / D - 0.5))
    jitter = jnp.exp(jax.random.uniform(pieces[1], (D,), jnp.float32, -1.15, 1.15))
    return (base * ramp * jitter).astype(jnp.bfloat16)


def draw_forgetting_speed_exponent(key, part):
    pieces = jax.random.split(key, 3)
    share = 0.5
    quick_pick = jax.random.uniform(pieces[0], (2, HEADS), jnp.float32) < share
    quick = math.log(math.log(10.0) / 50.0) + jax.random.uniform(pieces[1], (2, HEADS), jnp.float32, math.log(0.6), math.log(1.6))
    gentle = math.log(math.log(10.0) / (8 * TOK_DEV)) + jax.random.uniform(pieces[2], (2, HEADS), jnp.float32, math.log(0.2), 0.0)
    return jnp.where(quick_pick, quick, gentle).astype(jnp.float32)


def draw_forget_preacts(key, part):
    pieces = jax.random.split(key, 2)
    block_count = TOKENS // TOK_DEV
    offset = jax.random.uniform(pieces[0], (2, block_count, 1, HEADS), jnp.float32, -1.2, 1.2)
    noise = 0.6 * jnp.clip(jax.random.normal(pieces[1], (2, block_count, TOK_DEV, HEADS), jnp.float32), -6.0, 6.0)
    return (noise + offset).reshape(2, TOKENS, HEADS).astype(jnp.float32)


def draw_extra_forgetting_spikes(key, part):
    pieces = jax.random.split(key, 2)
    struck = jax.random.bernoulli(pieces[0], 1.0 / (2 * TOK_DEV), (2, TOKENS, HEADS))
    depth = jnp.log(jax.random.uniform(pieces[1], (2, TOKENS, HEADS), jnp.float32, 0.5, 0.8))
    return jnp.where(struck, depth, 0.0).astype(jnp.float32)


def steps_of(stream_key, shape, cuts, smallest, largest):
    def one(axis_at, shards_of):
        steps = jax.random.uniform(jax.random.fold_in(jax.random.fold_in(stream_key, 6), axis_at), (shards_of,), jnp.float32, smallest / len(cuts), largest / len(cuts))
        return jnp.repeat(jnp.exp(steps), shape[axis_at] // shards_of).reshape((-1,) + (1,) * (len(shape) - axis_at - 1))

    level = one(*cuts[0])
    for cut in cuts[1:]:
        level = level * one(*cut)
    return level


def profile(count, total, limit, slope):
    weights = [(1 << 20) // math.isqrt(grade ** slope) + 1 for grade in range(2, count + 1)]
    surplus, given = total - limit - (count - 1), [1] * (count - 1)
    while surplus > 0:
        free = [i for i in range(count - 1) if given[i] < limit]
        pool, budget = sum([weights[i] for i in free]), surplus
        for i in free:
            more = min(limit - given[i], max(1, budget * weights[i] // pool), surplus)
            given[i] = given[i] + more
            surplus = surplus - more
    return np.array([limit] + given)


def ragged_sizes(rng, count, total, reach, slope):
    if count == 2:
        one = jax.random.randint(rng, (), max(1, total - reach), min(reach, total - 1) + 1)
        return jnp.stack([one, total - one])
    sizes = jnp.asarray(profile(count, total, reach, slope), jnp.int32)
    twos = (count - 1) // 2
    source_of, receiver = sizes[1:1 + 2 * twos:2], sizes[2:2 + 2 * twos:2]
    room = jnp.minimum(source_of - 1, reach - receiver)
    moved = jax.random.randint(jax.random.fold_in(rng, 1), (twos,), 0, 1 << 20) % (room + 1)
    sizes = sizes.at[1:1 + 2 * twos:2].set(source_of - moved).at[2:2 + 2 * twos:2].set(receiver + moved)
    return sizes[jax.random.permutation(jax.random.fold_in(rng, 2), count)]


def centred(own_key, shape, width, most, shards=(), kind=jnp.bfloat16):
    level = steps_of(own_key, shape, shards, -0.22, 0.18) if shards else 1.0
    entries = jax.random.normal(own_key, shape, jnp.float32) * width * level
    return jnp.minimum(jnp.maximum(entries, -most), most).astype(kind)


def setup_inputs(seed: int = 0) -> dict:
    splits = jax.random.split(jax.random.key(seed), 15)
    skip_path_inputs = draw_skip_path_inputs(jax.random.fold_in(splits[14], 71), 0)
    probe_vectors = centred(splits[1], (TOKENS, HEADS * HEAD), 1.0, 6.0, ((0, 64), (1, 8)))
    lookup_vectors = centred(splits[2], (TOKENS, HEADS * HEAD), 1.0, 6.0, ((0, 64), (1, 8)))
    payload_vectors = centred(splits[3], (TOKENS, HEADS * HEAD), 1.0, 6.0, ((0, 64), (1, 8)))
    learning_strength_preacts = centred(splits[4], (2, TOKENS, HEADS), 1.5, 6.0, ((1, 64), (2, 8)), jnp.float32)
    forget_preacts = draw_forget_preacts(jax.random.fold_in(splits[14], 71), 0)
    forgetting_speed_exponent = draw_forgetting_speed_exponent(jax.random.fold_in(splits[14], 71), 0)
    extra_forgetting_spikes = draw_extra_forgetting_spikes(jax.random.fold_in(splits[14], 71), 0)
    sample_membership = jnp.searchsorted(jnp.cumsum(ragged_sizes(splits[8], DOCS, TOKENS, DOC_MOST, 1)), jnp.arange(TOKENS), side="right").astype(jnp.int32)
    channel_group_scaling = jnp.clip(1.0 + 0.18 * jax.random.normal(splits[9], (HEAD,), jnp.float32), 0.1, 1.9)
    blend_exit_weights = centred(splits[10], (HEADS * HEAD, D), (HEADS * HEAD) ** -0.5, 0.1875, ((0, 8),))
    dense_block_scaling = jnp.clip(1.0 + 0.18 * jax.random.normal(splits[11], (D,), jnp.float32), 0.1, 1.9)
    widen_projection_weights = centred(splits[12], (D, FF), D ** -0.5, 0.125, ((0, 64), (1, 8)))
    shrink_projection_weights = centred(splits[13], (FF, D), FF ** -0.5, 0.0625, ((0, 8), (1, 64)))
    return {"skip_path_inputs": skip_path_inputs, "probe_vectors": probe_vectors, "lookup_vectors": lookup_vectors, "payload_vectors": payload_vectors, "learning_strength_preacts": learning_strength_preacts, "forget_preacts": forget_preacts, "forgetting_speed_exponent": forgetting_speed_exponent, "extra_forgetting_spikes": extra_forgetting_spikes, "sample_membership": sample_membership, "channel_group_scaling": channel_group_scaling, "blend_exit_weights": blend_exit_weights, "dense_block_scaling": dense_block_scaling, "widen_projection_weights": widen_projection_weights, "shrink_projection_weights": shrink_projection_weights}


HIGH = lax.Precision.HIGHEST
EPSILON = 1e-06

def block_pass(memory, probe_vectors, lookup_vectors, payload_vectors, strengths, forget_multipliers, doc_ids, prior_doc, wanted):
    value_width = payload_vectors.shape[-1]
    block_len = probe_vectors.shape[1]
    running = jnp.cumsum(forget_multipliers, axis=-1)
    row_ids = lax.broadcasted_iota(jnp.int32, (block_len, block_len), 0)
    col_ids = lax.broadcasted_iota(jnp.int32, (block_len, block_len), 1)
    shared = doc_ids[:, None] == doc_ids[None, :]
    within = (row_ids >= col_ids) & shared
    before = (row_ids > col_ids) & shared
    spread = jnp.exp(jnp.where(within, running[:, :, None] - running[:, None, :], -jnp.inf))
    linked = (doc_ids == prior_doc).astype(jnp.float32)
    ending = (doc_ids == doc_ids[-1]).astype(jnp.float32)
    weighted = lookup_vectors * strengths[..., None]
    system = jnp.eye(block_len, dtype=jnp.float32) + jnp.where(before, jnp.einsum('hik,hjk->hij', weighted, lookup_vectors, precision=HIGH) * spread, 0.0)
    right_side = jnp.concatenate([payload_vectors * strengths[..., None], weighted * (jnp.exp(running) * linked)[..., None]], axis=-1)
    solved = jax.scipy.linalg.solve_triangular(system, right_side, lower=True, unit_diagonal=True)
    update = solved[..., :value_width] - jnp.einsum('hck,hkw->hcw', solved[..., value_width:], memory, precision=HIGH)
    faded_keys = lookup_vectors * (jnp.exp(running[:, -1:] - running) * ending)[..., None]
    kept_share = jnp.exp(running[:, -1]) * linked[-1]
    renewed = memory * kept_share[:, None, None] + jnp.einsum('hck,hcw->hkw', faded_keys, update, precision=HIGH)
    if not wanted:
        return (renewed, None)
    scores = jnp.where(within, jnp.einsum('hik,hjk->hij', probe_vectors, lookup_vectors, precision=HIGH) * spread, 0.0)
    reading = jnp.einsum('hck,hkw->hcw', probe_vectors * (jnp.exp(running) * linked)[..., None], memory, precision=HIGH)
    return (renewed, reading + jnp.einsum('hij,hjw->hiw', scores, update, precision=HIGH))

def run_blocks(memory, prior_doc, probe_vectors, lookup_vectors, payload_vectors, strengths, forget_multipliers, doc_ids, wanted):
    head_count, length, key_width = probe_vectors.shape
    block_count = length // BLOCK

    def split_blocks(tensor):
        return jnp.moveaxis(tensor.reshape((head_count, block_count, BLOCK) + tensor.shape[2:]), 1, 0)

    def advance(carried, inputs):
        held, earlier_doc = carried
        query_block, key_block, value_block, gate_block, decay_block, doc_block = inputs
        held, produced = block_pass(held, query_block, key_block, value_block, gate_block, decay_block, doc_block, earlier_doc, wanted)
        return ((held, doc_block[-1]), produced)
    (final, _), produced = lax.scan(advance, (memory, prior_doc), (split_blocks(probe_vectors), split_blocks(lookup_vectors), split_blocks(payload_vectors), split_blocks(strengths), split_blocks(forget_multipliers), doc_ids.reshape(block_count, BLOCK)))
    if wanted:
        produced = jnp.moveaxis(produced, 0, 1).reshape(head_count, length, -1)
    return (final, produced)

def unit_rows(tensor):
    return tensor * lax.rsqrt(lax.optimization_barrier(jnp.sum(tensor * tensor, axis=-1, keepdims=True)) + EPSILON)

def heads_first(tensor):
    row_count = tensor.shape[0]
    return jnp.transpose(tensor.astype(jnp.float32).reshape(row_count, HEADS, HEAD), (1, 0, 2))

def sweep(probe_vectors, lookup_vectors, payload_vectors, strengths, forget_multipliers, doc_ids):
    start_state = jnp.zeros((probe_vectors.shape[0], HEAD, HEAD), jnp.float32)
    _, produced = run_blocks(start_state, jnp.full((), -1, jnp.int32), probe_vectors, lookup_vectors, payload_vectors, strengths, forget_multipliers, doc_ids, True)
    return produced

def reference(skip_path_inputs, probe_vectors, lookup_vectors, payload_vectors, learning_strength_preacts, forget_preacts, forgetting_speed_exponent, extra_forgetting_spikes, sample_membership, channel_group_scaling, blend_exit_weights, dense_block_scaling, widen_projection_weights, shrink_projection_weights):
    length = probe_vectors.shape[0]
    query_heads = unit_rows(heads_first(probe_vectors)) * HEAD ** (-0.5)
    key_heads = unit_rows(heads_first(lookup_vectors))
    value_heads = heads_first(payload_vectors)
    strengths = jnp.transpose(jax.nn.sigmoid(learning_strength_preacts), (0, 2, 1))
    forget_multipliers = jnp.transpose(-jnp.exp(forgetting_speed_exponent)[:, None, :] * jax.nn.softplus(forget_preacts) + extra_forgetting_spikes, (0, 2, 1))
    forward_out = sweep(query_heads, key_heads, value_heads, strengths[0], forget_multipliers[0], sample_membership)
    backward_out = sweep(jnp.flip(query_heads, 1), jnp.flip(key_heads, 1), jnp.flip(value_heads, 1), jnp.flip(strengths[1], 1), jnp.flip(forget_multipliers[1], 1), jnp.flip(sample_membership, 0))
    attn = forward_out + jnp.flip(backward_out, 1)
    scaled = attn * lax.rsqrt(lax.optimization_barrier(jnp.mean(attn * attn, axis=-1, keepdims=True)) + EPSILON) * channel_group_scaling
    mixed = jnp.transpose(scaled, (1, 0, 2)).reshape(length, HEADS * HEAD).astype(jnp.bfloat16)
    group_width = HEADS * HEAD // N_TP
    projected = jnp.zeros((length, D), jnp.float32)
    for member in range(N_TP):
        group_term = jnp.dot(mixed[:, member * group_width:(member + 1) * group_width].astype(jnp.float32), blend_exit_weights[member * group_width:(member + 1) * group_width].astype(jnp.float32), preferred_element_type=jnp.float32)
        projected = projected + lax.optimization_barrier(group_term.astype(jnp.bfloat16)).astype(jnp.float32)
    residual = skip_path_inputs.astype(jnp.float32) + projected
    normed = (residual * lax.rsqrt(lax.optimization_barrier(jnp.mean(residual * residual, axis=-1, keepdims=True)) + EPSILON) * dense_block_scaling).astype(jnp.bfloat16)
    unit_width = FF // N_TP
    lowered = jnp.zeros((length, D), jnp.float32)
    for member in range(N_TP):
        raised = jnp.dot(normed.astype(jnp.float32), widen_projection_weights[:, member * unit_width:(member + 1) * unit_width].astype(jnp.float32), preferred_element_type=jnp.float32)
        active = jnp.square(jax.nn.relu(raised)).astype(jnp.bfloat16)
        group_term = jnp.dot(active.astype(jnp.float32), shrink_projection_weights[member * unit_width:(member + 1) * unit_width].astype(jnp.float32), preferred_element_type=jnp.float32)
        lowered = lowered + lax.optimization_barrier(group_term.astype(jnp.bfloat16)).astype(jnp.float32)
    return (residual + lowered).astype(jnp.bfloat16)
```

```python
import jax
import jax.numpy as jnp
from jax import lax
from jax.experimental import pallas as pl
from jax.experimental.pallas import tpu as pltpu
from jax.sharding import Mesh
from jax.sharding import PartitionSpec as P

SP = ("sp_0", "sp_1")
EPSILON = 1e-06
F32 = jnp.float32
BF16 = jnp.bfloat16
NT = (((1,), (1,)), ((), ()))
NN = (((1,), (0,)), ((), ()))


def mm(a, b, dims=NN):
    return lax.dot_general(a.astype(BF16), b.astype(BF16), dims, preferred_element_type=F32)


def split_in_two(a):
    high = a.astype(BF16)
    return high, (a - high.astype(F32)).astype(BF16)


def mm2(a, b, dims=NN):
    high, low = split_in_two(a)
    return mm(high, b, dims) + mm(low, b, dims)


def mm3(a, b):
    a_high, a_low = split_in_two(a)
    b_high, b_low = split_in_two(b)
    return mm(a_high, b_high) + (mm(a_high, b_low) + mm(a_low, b_high))


def local_kernel(
    q_ref, k_ref, v_ref, gates_ref, speed_ref, docs_ref, fwd_ref, bwd_ref, read_ref, own_ref
):
    n, width = q_ref.shape
    q, k, v = q_ref[...], k_ref[...], v_ref[...]
    rows = lax.broadcasted_iota(jnp.int32, (n, n), 0)
    cols = lax.broadcasted_iota(jnp.int32, (n, n), 1)
    eye = rows == cols

    def to_col(row):
        return jnp.sum(jnp.where(eye, row, 0.0), axis=1, keepdims=True)

    def to_row(col):
        return jnp.sum(jnp.where(eye, col, 0.0), axis=0, keepdims=True)

    gates = gates_ref[...]
    betas = jax.nn.sigmoid(gates[0:2])
    preacts = gates[2:4]
    soft = jnp.maximum(preacts, 0.0) + jnp.log1p(jnp.exp(-jnp.abs(preacts)))
    decays = -jnp.exp(speed_ref[...]) * soft + gates[4:6]
    docs_row = docs_ref[...].astype(F32)
    docs_col = to_col(docs_row)
    shared = docs_col == docs_row
    qf, kf = q.astype(F32), k.astype(F32)
    q_scale = lax.rsqrt(jnp.sum(qf * qf, axis=1, keepdims=True) + EPSILON) * width ** (-0.5)
    k_scale = lax.rsqrt(jnp.sum(kf * kf, axis=1, keepdims=True) + EPSILON)
    k_scale_row = to_row(k_scale)
    similar = mm(k, k, NT) * k_scale * k_scale_row
    scored = mm(q, k, NT) * q_scale * k_scale_row
    k_turned = jnp.transpose(kf)
    near = [((rows ^ cols) >> lg) == 1 for lg in range(7)]
    outputs = 0.0
    for way, message_ref in ((0, fwd_ref), (1, bwd_ref)):
        first, last = (0, n - 1) if way == 0 else (n - 1, 0)
        reach = (rows >= cols) if way == 0 else (rows <= cols)
        decay_row = decays[way : way + 1]
        beta_row = betas[way : way + 1]
        running = jnp.sum(jnp.where(reach, decay_row, 0.0), axis=1, keepdims=True)
        running_row = to_row(running)
        within = reach & shared
        spread = jnp.exp(jnp.where(within, running - running_row, -jnp.inf))
        strict = jnp.where(eye, 0.0, similar * spread * to_col(beta_row))
        inverse = jnp.where(eye, 1.0, 0.0) - jnp.where(near[0], strict, 0.0)
        for lg in range(1, 7):
            inverse = inverse - mm3(inverse, mm3(jnp.where(near[lg], strict, 0.0), inverse))
        linked_row = (docs_row == docs_row[:, first : first + 1]).astype(F32)
        linked = (docs_col == docs_col[first : first + 1]).astype(F32)
        ending_row = (docs_row == docs_row[:, last : last + 1]).astype(F32)
        total = running_row[:, last : last + 1]
        update = mm2(inverse * beta_row, v)
        mask = inverse * (beta_row * jnp.exp(running_row) * linked_row * k_scale_row)
        drop = mm2(mask, k)
        faded = k_turned * (k_scale_row * jnp.exp(total - running_row) * ending_row)
        kept = jnp.exp(total) * linked_row[:, last : last + 1]
        message_ref[:, :width] = jnp.where(eye, kept, 0.0) - mm(faded, drop)
        message_ref[:, width:] = mm(faded, update)
        scores = scored * spread
        queries = qf * (q_scale * jnp.exp(running) * linked)
        read_ref[way] = (queries - mm(scores, drop)).astype(BF16)
        outputs = outputs + mm(scores, update)
    own_ref[...] = outputs


def combine_kernel(fwd_ref, fwd_in_ref, bwd_ref, bwd_in_ref, fwd_out_ref, bwd_out_ref):
    for own_ref, in_ref, out_ref in (
        (fwd_ref, fwd_in_ref, fwd_out_ref),
        (bwd_ref, bwd_in_ref, bwd_out_ref),
    ):
        n = own_ref.shape[0]
        moved = mm(own_ref[:, :n], in_ref[...])
        out_ref[:, :n] = moved[:, :n].astype(BF16)
        out_ref[:, n:] = (moved[:, n:] + own_ref[:, n:].astype(F32)).astype(BF16)


def finish_kernel(
    own_ref, read_ref, fwd_ref, fwd_far_ref, bwd_ref, bwd_far_ref, links_ref, gain_ref, exit_ref, out_ref
):
    n = own_ref.shape[0]
    attn = own_ref[...]
    for way, near_ref, far_ref in ((0, fwd_ref, fwd_far_ref), (1, bwd_ref, bwd_far_ref)):
        state = mm(near_ref[:, :n], far_ref[...]) + near_ref[:, n:].astype(F32)
        attn = attn + mm(read_ref[way], state * links_ref[way : way + 1])
    mean = jnp.mean(attn * attn, axis=1, keepdims=True)
    mixed = (attn * lax.rsqrt(mean + EPSILON) * gain_ref[...]).astype(BF16)
    terms = mm(mixed, exit_ref[...]).astype(BF16)
    step = out_ref.shape[2]
    for m in range(out_ref.shape[0]):
        out_ref[m] = terms[:, m * step : (m + 1) * step]


def vmem(count):
    return [pl.BlockSpec(memory_space=pltpu.VMEM)] * count


def shards(
    skip_path_inputs,
    probe_vectors,
    lookup_vectors,
    payload_vectors,
    learning_strength_preacts,
    forget_preacts,
    forgetting_speed_exponent,
    extra_forgetting_spikes,
    sample_membership,
    channel_group_scaling,
    blend_exit_weights,
    dense_block_scaling,
    widen_projection_weights,
    shrink_projection_weights,
):
    up_width = widen_projection_weights.shape[1]
    weights = lax.all_gather(
        jnp.concatenate([widen_projection_weights, shrink_projection_weights.T], axis=1),
        SP,
        axis=0,
        tiled=True,
    )
    length, width = probe_vectors.shape
    count = lax.axis_size(SP)

    def passed(array, distance):
        pairs = [(i, (i + distance) % count) for i in range(count)]
        return lax.ppermute(array, SP, pairs)

    docs = sample_membership.reshape(1, length)
    prior = passed(docs, 1)
    later = passed(docs, -1)
    gates = jnp.concatenate(
        [
            learning_strength_preacts.reshape(2, length),
            forget_preacts.reshape(2, length),
            extra_forgetting_spikes.reshape(2, length),
        ]
    )
    square = (width, width)
    pair = (width, 2 * width)
    fwd, bwd, read, own = pl.pallas_call(
        local_kernel,
        out_shape=(
            jax.ShapeDtypeStruct(pair, F32),
            jax.ShapeDtypeStruct(pair, F32),
            jax.ShapeDtypeStruct((2, length, width), BF16),
            jax.ShapeDtypeStruct((length, width), F32),
        ),
        in_specs=vmem(6),
        out_specs=tuple(vmem(4)),
        name="local_maps",
    )(
        probe_vectors,
        lookup_vectors,
        payload_vectors,
        gates,
        forgetting_speed_exponent,
        docs,
    )
    fwd_link = (prior[0, length - 1] == docs[0, 0]).astype(F32)
    bwd_link = (later[0, 0] == docs[0, length - 1]).astype(F32)
    is_map = lax.broadcasted_iota(jnp.int32, pair, 1) < width
    fwd = (fwd * jnp.where(is_map, fwd_link, 1.0)).astype(BF16)
    bwd = (bwd * jnp.where(is_map, bwd_link, 1.0)).astype(BF16)
    links = jnp.broadcast_to(jnp.stack([fwd_link, bwd_link])[:, None], (2, width))
    for distance in (1, 2):
        fwd, bwd = pl.pallas_call(
            combine_kernel,
            out_shape=(jax.ShapeDtypeStruct(pair, BF16),) * 2,
            in_specs=vmem(4),
            out_specs=tuple(vmem(2)),
            name="combine_maps",
        )(fwd, passed(fwd, distance), bwd, passed(bwd, -distance))
    head_terms = pl.pallas_call(
        finish_kernel,
        out_shape=jax.ShapeDtypeStruct((8, length, blend_exit_weights.shape[1] // 8), BF16),
        in_specs=vmem(9),
        out_specs=vmem(1)[0],
        name="finish_mixer",
    )(
        own,
        read,
        passed(fwd, 1),
        passed(fwd[:, width:], 5),
        passed(bwd, -1),
        passed(bwd[:, width:], -5),
        links,
        channel_group_scaling.reshape(1, width),
        blend_exit_weights,
    )
    model_width = skip_path_inputs.shape[1]
    col_count = model_width // lax.axis_size("tp")
    col_start = lax.axis_index("tp") * col_count
    parts = lax.all_to_all(head_terms, "tp", 0, 0, tiled=True)
    own_residual = lax.dynamic_slice_in_dim(skip_path_inputs, col_start, col_count, 1).astype(
        F32
    ) + jnp.sum(parts.astype(F32), axis=0)
    residual = lax.all_gather(own_residual.astype(BF16), "tp", axis=1, tiled=True).astype(F32)
    squares = jnp.mean(residual * residual, axis=1, keepdims=True)
    normed = (residual * lax.rsqrt(squares + EPSILON) * dense_block_scaling).astype(BF16)
    raised = jnp.dot(normed, weights[:, :up_width], preferred_element_type=F32)
    active = jnp.square(jax.nn.relu(raised)).astype(BF16)
    lowered = lax.dot_general(active, weights[:, up_width:], NT, preferred_element_type=F32)
    turned = jnp.moveaxis(lowered.astype(BF16).reshape(length, -1, col_count), 1, 0)
    pieces = lax.all_to_all(turned, "tp", 0, 0, tiled=True)
    return (own_residual + jnp.sum(pieces.astype(F32), axis=0)).astype(BF16)


def solution(mesh):
    torus = Mesh(mesh.devices.reshape(8, 8, mesh.shape["tp"]), ("sp_0", "sp_1", "tp"))
    placed = (
        P(SP, None),
        P(SP, "tp"),
        P(SP, "tp"),
        P(SP, "tp"),
        P(None, SP, "tp"),
        P(None, SP, "tp"),
        P(None, "tp"),
        P(None, SP, "tp"),
        P(SP),
        P(),
        P("tp", None),
        P(),
        P(SP, "tp"),
        P("tp", SP),
    )
    return jax.shard_map(
        shards, mesh=torus, in_specs=placed, out_specs=P(SP, "tp"), check_vma=False
    )
```

```python
import jax
import jax.numpy as jnp
from jax import lax
from jax.experimental import pallas as pl
from jax.experimental.pallas import tpu as pltpu
from jax.sharding import Mesh
from jax.sharding import PartitionSpec as P

SP = ("sp_0", "sp_1")
EPSILON = 1e-06
F32 = jnp.float32
BF16 = jnp.bfloat16
NT = (((1,), (1,)), ((), ()))
NN = (((1,), (0,)), ((), ()))


def mm(a, b, dims=NN):
    return lax.dot_general(a.astype(BF16), b.astype(BF16), dims, preferred_element_type=F32)


def split_in_two(a):
    high = a.astype(BF16)
    return high, (a - high.astype(F32)).astype(BF16)


def mm2(a, b, dims=NN):
    high, low = split_in_two(a)
    return mm(high, b, dims) + mm(low, b, dims)


def mm3(a, b):
    a_high, a_low = split_in_two(a)
    b_high, b_low = split_in_two(b)
    return mm(a_high, b_high) + (mm(a_high, b_low) + mm(a_low, b_high))


def local_kernel(own_ref, own_rows_ref, pal_ref, pal_rows_ref, message_ref, read_ref, base_ref):
    n = own_ref.shape[0]
    width = own_ref.shape[1] // 3
    back = lax.axis_index("sp_1") % 2
    sign = 1 - 2 * back
    forward = back == 0
    rows = lax.broadcasted_iota(jnp.int32, (n, n), 0)
    cols = lax.broadcasted_iota(jnp.int32, (n, n), 1)
    eye = rows == cols
    reach = (rows - cols) * sign >= 0
    near = [((rows ^ cols) >> lg) == 1 for lg in range(7)]

    def to_col(row):
        return jnp.sum(jnp.where(eye, row, 0.0), axis=1, keepdims=True)

    def to_row(col):
        return jnp.sum(jnp.where(eye, col, 0.0), axis=0, keepdims=True)

    def chosen(pair):
        return jnp.where(forward, pair[0:1], pair[1:2])

    def block(data_ref, rows_ref):
        q, k, v = (data_ref[:, m * width : (m + 1) * width] for m in range(3))
        gates = rows_ref[...]
        beta_row = jax.nn.sigmoid(chosen(gates[0:2]))
        preacts = chosen(gates[2:4])
        soft = jnp.maximum(preacts, 0.0) + jnp.log1p(jnp.exp(-jnp.abs(preacts)))
        speed = jnp.where(forward, gates[7:8, 0:1], gates[7:8, n - 1 : n])
        decay_row = -jnp.exp(speed) * soft + chosen(gates[4:6])
        docs_row = gates[6:7]
        docs_first = jnp.where(forward, docs_row[:, 0:1], docs_row[:, n - 1 : n])
        docs_last = jnp.where(forward, docs_row[:, n - 1 : n], docs_row[:, 0:1])
        docs_col = to_col(docs_row)
        qf, kf = q.astype(F32), k.astype(F32)
        q_scale = lax.rsqrt(jnp.sum(qf * qf, axis=1, keepdims=True) + EPSILON) * width ** (-0.5)
        k_scale = lax.rsqrt(jnp.sum(kf * kf, axis=1, keepdims=True) + EPSILON)
        k_scale_row = to_row(k_scale)
        similar = mm(k, k, NT) * k_scale * k_scale_row
        scored = mm(q, k, NT) * q_scale * k_scale_row
        running = jnp.sum(jnp.where(reach, decay_row, 0.0), axis=1, keepdims=True)
        running_row = to_row(running)
        total = jnp.sum(decay_row, axis=1, keepdims=True)
        within = reach & (docs_col == docs_row)
        spread = jnp.exp(jnp.where(within, running - running_row, -jnp.inf))
        strict = jnp.where(eye, 0.0, similar * spread * to_col(beta_row))
        inverse = jnp.where(eye, 1.0, 0.0) - jnp.where(near[0], strict, 0.0)
        for lg in range(1, 7):
            inverse = inverse - mm3(inverse, mm3(jnp.where(near[lg], strict, 0.0), inverse))
        linked_row = (docs_row == docs_first).astype(F32)
        linked = (docs_col == docs_first).astype(F32)
        ending_row = (docs_row == docs_last).astype(F32)
        update = mm2(inverse * beta_row, v)
        drop = mm2(inverse * (beta_row * jnp.exp(running_row) * linked_row * k_scale_row), k)
        tail = jnp.exp(jnp.minimum(total - running_row, 0.0))
        faded = jnp.transpose(kf) * (k_scale_row * tail * ending_row)
        kept = jnp.exp(total) * (docs_first == docs_last).astype(F32)
        step = jnp.where(eye, kept, 0.0) - mm(faded, drop)
        shift = mm(faded, update)
        scores = scored * spread
        read = qf * (q_scale * jnp.exp(running) * linked) - mm(scores, drop)
        return step, shift, read, mm(scores, update), docs_first, docs_last

    step, shift, read, base, docs_first, docs_mid = block(own_ref, own_rows_ref)
    pal_step, pal_shift, pal_read, pal_base, docs_next, docs_last = block(pal_ref, pal_rows_ref)
    link = (docs_mid == docs_next).astype(F32)
    step, shift = step * link, shift * link
    message_ref[:n, :width] = mm(pal_step, step).astype(BF16)
    message_ref[:n, width:] = (mm(pal_step, shift) + pal_shift).astype(BF16)
    mark_docs(message_ref, n, docs_first, docs_last)
    read_ref[0] = read.astype(BF16)
    read_ref[1] = mm(pal_read, step).astype(BF16)
    base_ref[0] = base
    base_ref[1] = pal_base + mm(pal_read, shift)


def mark_docs(ref, n, docs_first, docs_last):
    ref[n : n + 8] = jnp.broadcast_to(docs_first, (8, ref.shape[1])).astype(BF16)
    ref[n + 8 :] = jnp.broadcast_to(docs_last, (8, ref.shape[1])).astype(BF16)


def combine_kernel(own_ref, in_ref, out_ref, far_ref):
    n = own_ref.shape[0] - 16
    docs_first = own_ref[n : n + 8, 0:1][0:1].astype(F32)
    in_last = in_ref[n + 8 :, 0:1][0:1].astype(F32)
    link = (docs_first == in_last).astype(F32)
    moved = mm(own_ref[:n, :n], in_ref[:n, :]) * link
    shift = (moved[:, n:] + own_ref[:n, n:].astype(F32)).astype(BF16)
    out_ref[:n, :n] = moved[:, :n].astype(BF16)
    out_ref[:n, n:] = shift
    out_ref[n : n + 8] = in_ref[n : n + 8]
    out_ref[n + 8 :] = own_ref[n + 8 :]
    far_ref[:n] = shift
    far_ref[n : n + 8] = in_ref[n : n + 8, :n]
    far_ref[n + 8 :] = own_ref[n + 8 :, :n]


def apply_kernel(own_ref, near_ref, far_ref, read_ref, base_ref, mine_ref, other_ref):
    n = own_ref.shape[0] - 16
    docs_first = own_ref[n : n + 8, 0:1][0:1].astype(F32)
    near_first = near_ref[n : n + 8, 0:1][0:1].astype(F32)
    near_last = near_ref[n + 8 :, 0:1][0:1].astype(F32)
    far_last = far_ref[n + 8 :, 0:1][0:1].astype(F32)
    state = mm(near_ref[:n, :n], far_ref[:n]) * (near_first == far_last).astype(F32)
    state = (state + near_ref[:n, n:].astype(F32)) * (docs_first == near_last).astype(F32)
    other_ref[...] = (base_ref[1] + mm(read_ref[1], state)).astype(BF16)
    mine_ref[...] = base_ref[0] + mm(read_ref[0], state)


def finish_kernel(mine_ref, in_ref, gain_ref, exit_ref, out_ref):
    attn = mine_ref[...] + in_ref[...].astype(F32)
    mean = jnp.mean(attn * attn, axis=1, keepdims=True)
    mixed = (attn * lax.rsqrt(mean + EPSILON) * gain_ref[...]).astype(BF16)
    terms = mm(mixed, exit_ref[...]).astype(BF16)
    step = out_ref.shape[2]
    for m in range(out_ref.shape[0]):
        out_ref[m] = terms[:, m * step : (m + 1) * step]


def vmem(count):
    return [pl.BlockSpec(memory_space=pltpu.VMEM)] * count


def shards(
    skip_path_inputs,
    probe_vectors,
    lookup_vectors,
    payload_vectors,
    learning_strength_preacts,
    forget_preacts,
    forgetting_speed_exponent,
    extra_forgetting_spikes,
    sample_membership,
    channel_group_scaling,
    blend_exit_weights,
    dense_block_scaling,
    widen_projection_weights,
    shrink_projection_weights,
):
    up_width = widen_projection_weights.shape[1]
    weights = lax.all_gather(
        jnp.concatenate([widen_projection_weights, shrink_projection_weights.T], axis=1),
        SP,
        axis=0,
        tiled=True,
    )
    length, width = probe_vectors.shape
    count = lax.axis_size(SP)

    def swapped(array):
        return lax.ppermute(array, SP, [(i, i ^ 1) for i in range(count)])

    def passed(array, distance):
        ways = (2 * distance, -2 * distance)
        return lax.ppermute(array, SP, [(i, (i + ways[i % 2]) % count) for i in range(count)])

    data = jnp.concatenate([probe_vectors, lookup_vectors, payload_vectors], axis=1)
    lanes = lax.broadcasted_iota(jnp.int32, (1, length), 1)
    rows = jnp.concatenate(
        [
            learning_strength_preacts.reshape(2, length),
            forget_preacts.reshape(2, length),
            extra_forgetting_spikes.reshape(2, length),
            sample_membership.astype(F32).reshape(1, length),
            jnp.where(
                lanes < length // 2,
                forgetting_speed_exponent[0:1],
                forgetting_speed_exponent[1:2],
            ),
        ]
    )
    tall = width + 16
    message, read, base = pl.pallas_call(
        local_kernel,
        out_shape=(
            jax.ShapeDtypeStruct((tall, 2 * width), BF16),
            jax.ShapeDtypeStruct((2, length, width), BF16),
            jax.ShapeDtypeStruct((2, length, width), F32),
        ),
        in_specs=vmem(4),
        out_specs=tuple(vmem(3)),
        name="local_maps",
    )(data, rows, swapped(data), swapped(rows))
    joined, far = pl.pallas_call(
        combine_kernel,
        out_shape=(
            jax.ShapeDtypeStruct((tall, 2 * width), BF16),
            jax.ShapeDtypeStruct((tall, width), BF16),
        ),
        in_specs=vmem(2),
        out_specs=tuple(vmem(2)),
        name="combine_maps",
    )(message, passed(message, 1))
    mine, other = pl.pallas_call(
        apply_kernel,
        out_shape=(
            jax.ShapeDtypeStruct((length, width), F32),
            jax.ShapeDtypeStruct((length, width), BF16),
        ),
        in_specs=vmem(5),
        out_specs=tuple(vmem(2)),
        name="apply_state",
    )(message, passed(joined, 1), passed(far, 3), read, base)
    head_terms = pl.pallas_call(
        finish_kernel,
        out_shape=jax.ShapeDtypeStruct((8, length, blend_exit_weights.shape[1] // 8), BF16),
        in_specs=vmem(4),
        out_specs=vmem(1)[0],
        name="finish_mixer",
    )(mine, swapped(other), channel_group_scaling.reshape(1, width), blend_exit_weights)
    model_width = skip_path_inputs.shape[1]
    col_count = model_width // lax.axis_size("tp")
    col_start = lax.axis_index("tp") * col_count
    parts = lax.all_to_all(head_terms, "tp", 0, 0, tiled=True)
    own_residual = lax.dynamic_slice_in_dim(skip_path_inputs, col_start, col_count, 1).astype(
        F32
    ) + jnp.sum(parts.astype(F32), axis=0)
    residual = lax.all_gather(own_residual.astype(BF16), "tp", axis=1, tiled=True).astype(F32)
    squares = jnp.mean(residual * residual, axis=1, keepdims=True)
    normed = (residual * lax.rsqrt(squares + EPSILON) * dense_block_scaling).astype(BF16)
    raised = jnp.dot(normed, weights[:, :up_width], preferred_element_type=F32)
    active = jnp.square(jax.nn.relu(raised)).astype(BF16)
    lowered = lax.dot_general(active, weights[:, up_width:], NT, preferred_element_type=F32)
    turned = jnp.moveaxis(lowered.astype(BF16).reshape(length, -1, col_count), 1, 0)
    pieces = lax.all_to_all(turned, "tp", 0, 0, tiled=True)
    return (own_residual + jnp.sum(pieces.astype(F32), axis=0)).astype(BF16)


def solution(mesh):
    torus = Mesh(mesh.devices.reshape(8, 8, mesh.shape["tp"]), ("sp_0", "sp_1", "tp"))
    placed = (
        P(SP, None),
        P(SP, "tp"),
        P(SP, "tp"),
        P(SP, "tp"),
        P(None, SP, "tp"),
        P(None, SP, "tp"),
        P(None, "tp"),
        P(None, SP, "tp"),
        P(SP),
        P(),
        P("tp", None),
        P(),
        P(SP, "tp"),
        P("tp", SP),
    )
    return jax.shard_map(
        shards, mesh=torus, in_specs=placed, out_specs=P(SP, "tp"), check_vma=False
    )
```

```python
import jax
import jax.numpy as jnp
from jax import lax
from jax.experimental import pallas as pl
from jax.experimental.pallas import tpu as pltpu
from jax.sharding import Mesh
from jax.sharding import PartitionSpec as P

SP = ("sp_0", "sp_1", "pair")
EPSILON = 1e-06
F32 = jnp.float32
BF16 = jnp.bfloat16
NT = (((1,), (1,)), ((), ()))
NN = (((1,), (0,)), ((), ()))


def mm(a, b, dims=NN):
    return lax.dot_general(a.astype(BF16), b.astype(BF16), dims, preferred_element_type=F32)


def split_in_two(a):
    high = a.astype(BF16)
    return high, (a - high.astype(F32)).astype(BF16)


def mm2(a, b, dims=NN):
    high, low = split_in_two(a)
    return mm(high, b, dims) + mm(low, b, dims)


def mm3(a, b):
    a_high, a_low = split_in_two(a)
    b_high, b_low = split_in_two(b)
    return mm(a_high, b_high) + (mm(a_high, b_low) + mm(a_low, b_high))


def pack_kernel(q_ref, k_ref, v_ref, strength_ref, forget_ref, spike_ref, docs_ref, out_ref):
    n, width = q_ref.shape
    for m, ref in enumerate((q_ref, k_ref, v_ref)):
        out_ref[:n, m * width : (m + 1) * width] = ref[...]
    docs = docs_ref[...].astype(F32)
    rest = jnp.concatenate([strength_ref[...], forget_ref[...], spike_ref[...], docs, docs])
    for m in range(3):
        piece = rest.astype(BF16)
        out_ref[n:, m * width : (m + 1) * width] = piece
        rest = rest - piece.astype(F32)


def local_kernel(own_ref, pal_ref, speed_ref, message_ref, read_ref, base_ref):
    n = own_ref.shape[0] - 8
    width = own_ref.shape[1] // 3
    back = lax.axis_index("pair")
    sign = 1 - 2 * back
    forward = back == 0
    rows = lax.broadcasted_iota(jnp.int32, (n, n), 0)
    cols = lax.broadcasted_iota(jnp.int32, (n, n), 1)
    eye = rows == cols
    reach = (rows - cols) * sign >= 0
    near = [((rows ^ cols) >> lg) == 1 for lg in range(7)]

    def to_col(row):
        return jnp.sum(jnp.where(eye, row, 0.0), axis=1, keepdims=True)

    def to_row(col):
        return jnp.sum(jnp.where(eye, col, 0.0), axis=0, keepdims=True)

    def chosen(pair):
        return jnp.where(forward, pair[0:1], pair[1:2])

    def block(data_ref):
        q, k, v = (data_ref[:n, m * width : (m + 1) * width] for m in range(3))
        high, middle, low = (
            data_ref[n:, m * width : (m + 1) * width].astype(F32) for m in range(3)
        )
        gates = (low + middle) + high
        beta_row = jax.nn.sigmoid(chosen(gates[0:2]))
        preacts = chosen(gates[2:4])
        soft = jnp.maximum(preacts, 0.0) + jnp.log1p(jnp.exp(-jnp.abs(preacts)))
        speed = jnp.where(forward, speed_ref[:, 0:1], speed_ref[:, 1:2])
        decay_row = -jnp.exp(speed) * soft + chosen(gates[4:6])
        docs_row = gates[6:7]
        docs_first = jnp.where(forward, docs_row[:, 0:1], docs_row[:, n - 1 : n])
        docs_last = jnp.where(forward, docs_row[:, n - 1 : n], docs_row[:, 0:1])
        docs_col = to_col(docs_row)
        qf, kf = q.astype(F32), k.astype(F32)
        q_scale = lax.rsqrt(jnp.sum(qf * qf, axis=1, keepdims=True) + EPSILON) * width ** (-0.5)
        k_scale = lax.rsqrt(jnp.sum(kf * kf, axis=1, keepdims=True) + EPSILON)
        k_scale_row = to_row(k_scale)
        similar = mm(k, k, NT) * k_scale * k_scale_row
        scored = mm(q, k, NT) * q_scale * k_scale_row
        running = jnp.sum(jnp.where(reach, decay_row, 0.0), axis=1, keepdims=True)
        running_row = to_row(running)
        total = jnp.sum(decay_row, axis=1, keepdims=True)
        within = reach & (docs_col == docs_row)
        spread = jnp.exp(jnp.where(within, running - running_row, -jnp.inf))
        strict = jnp.where(eye, 0.0, similar * spread * to_col(beta_row))
        inverse = jnp.where(eye, 1.0, 0.0) - jnp.where(near[0], strict, 0.0)
        for lg in range(1, 7):
            inverse = inverse - mm3(inverse, mm3(jnp.where(near[lg], strict, 0.0), inverse))
        linked_row = (docs_row == docs_first).astype(F32)
        linked = (docs_col == docs_first).astype(F32)
        ending_row = (docs_row == docs_last).astype(F32)
        update = mm2(inverse * beta_row, v)
        drop = mm2(inverse * (beta_row * jnp.exp(running_row) * linked_row * k_scale_row), k)
        tail = jnp.exp(jnp.minimum(total - running_row, 0.0))
        faded = jnp.transpose(kf) * (k_scale_row * tail * ending_row)
        kept = jnp.exp(total) * (docs_first == docs_last).astype(F32)
        step = jnp.where(eye, kept, 0.0) - mm(faded, drop)
        shift = mm(faded, update)
        scores = scored * spread
        read = qf * (q_scale * jnp.exp(running) * linked) - mm(scores, drop)
        return step, shift, read, mm(scores, update), docs_first, docs_last

    step, shift, read, base, docs_first, docs_mid = block(own_ref)
    pal_step, pal_shift, pal_read, pal_base, docs_next, docs_last = block(pal_ref)
    link = (docs_mid == docs_next).astype(F32)
    step, shift = step * link, shift * link
    message_ref[:n, :width] = mm(pal_step, step).astype(BF16)
    message_ref[:n, width:] = (mm(pal_step, shift) + pal_shift).astype(BF16)
    mark_docs(message_ref, n, docs_first, docs_last)
    read_ref[0] = read.astype(BF16)
    read_ref[1] = mm(pal_read, step).astype(BF16)
    base_ref[0] = base
    base_ref[1] = pal_base + mm(pal_read, shift)


def mark_docs(ref, n, docs_first, docs_last):
    ref[n : n + 8] = jnp.broadcast_to(docs_first, (8, ref.shape[1])).astype(BF16)
    ref[n + 8 :] = jnp.broadcast_to(docs_last, (8, ref.shape[1])).astype(BF16)


def combine_kernel(own_ref, in_ref, out_ref, far_ref):
    n = own_ref.shape[0] - 16
    docs_first = own_ref[n : n + 8, 0:1][0:1].astype(F32)
    in_last = in_ref[n + 8 :, 0:1][0:1].astype(F32)
    link = (docs_first == in_last).astype(F32)
    moved = mm(own_ref[:n, :n], in_ref[:n, :]) * link
    shift = (moved[:, n:] + own_ref[:n, n:].astype(F32)).astype(BF16)
    out_ref[:n, :n] = moved[:, :n].astype(BF16)
    out_ref[:n, n:] = shift
    out_ref[n : n + 8] = in_ref[n : n + 8]
    out_ref[n + 8 :] = own_ref[n + 8 :]
    far_ref[:n] = shift
    far_ref[n : n + 8] = in_ref[n : n + 8, :n]
    far_ref[n + 8 :] = own_ref[n + 8 :, :n]


def apply_kernel(own_ref, near_ref, far_ref, read_ref, base_ref, mine_ref, other_ref):
    n = own_ref.shape[0] - 16
    docs_first = own_ref[n : n + 8, 0:1][0:1].astype(F32)
    near_first = near_ref[n : n + 8, 0:1][0:1].astype(F32)
    near_last = near_ref[n + 8 :, 0:1][0:1].astype(F32)
    far_last = far_ref[n + 8 :, 0:1][0:1].astype(F32)
    state = mm(near_ref[:n, :n], far_ref[:n]) * (near_first == far_last).astype(F32)
    state = (state + near_ref[:n, n:].astype(F32)) * (docs_first == near_last).astype(F32)
    other_ref[...] = (base_ref[1] + mm(read_ref[1], state)).astype(BF16)
    mine_ref[...] = base_ref[0] + mm(read_ref[0], state)


def finish_kernel(mine_ref, in_ref, gain_ref, exit_ref, out_ref):
    attn = mine_ref[...] + in_ref[...].astype(F32)
    mean = jnp.mean(attn * attn, axis=1, keepdims=True)
    mixed = (attn * lax.rsqrt(mean + EPSILON) * gain_ref[...]).astype(BF16)
    terms = mm(mixed, exit_ref[...]).astype(BF16)
    step = out_ref.shape[2]
    for m in range(out_ref.shape[0]):
        out_ref[m] = terms[:, m * step : (m + 1) * step]


def vmem(count):
    return [pl.BlockSpec(memory_space=pltpu.VMEM)] * count


def shards(
    skip_path_inputs,
    probe_vectors,
    lookup_vectors,
    payload_vectors,
    learning_strength_preacts,
    forget_preacts,
    forgetting_speed_exponent,
    extra_forgetting_spikes,
    sample_membership,
    channel_group_scaling,
    blend_exit_weights,
    dense_block_scaling,
    widen_projection_weights,
    shrink_projection_weights,
):
    length, width = probe_vectors.shape
    count = lax.axis_size(SP)

    def swapped(array):
        return lax.ppermute(array, SP, [(i, i ^ 1) for i in range(count)])

    def passed(array, distance):
        ways = (2 * distance, -2 * distance)
        return lax.ppermute(array, SP, [(i, (i + ways[i % 2]) % count) for i in range(count)])

    data = pl.pallas_call(
        pack_kernel,
        out_shape=jax.ShapeDtypeStruct((length + 8, 3 * width), BF16),
        in_specs=vmem(7),
        out_specs=vmem(1)[0],
        name="pack_inputs",
    )(
        probe_vectors,
        lookup_vectors,
        payload_vectors,
        learning_strength_preacts.reshape(2, length),
        forget_preacts.reshape(2, length),
        extra_forgetting_spikes.reshape(2, length),
        sample_membership.reshape(1, length),
    )
    pal_data = swapped(data)
    side = lax.axis_index("pair")
    half = widen_projection_weights.shape[1] // 2

    def halves(which):
        return jnp.concatenate(
            [
                lax.dynamic_slice_in_dim(array, which * half, half, 1)
                for array in (widen_projection_weights, shrink_projection_weights.T)
            ],
            axis=1,
        )

    kept_half = halves(side)
    given_half = swapped(halves(1 - side))
    weights = lax.all_gather(
        jnp.concatenate(
            [
                jnp.where(side == 0, kept_half, given_half),
                jnp.where(side == 0, given_half, kept_half),
            ]
        ),
        SP[:2],
        axis=0,
        tiled=True,
    )
    tall = width + 16
    message, read, base = pl.pallas_call(
        local_kernel,
        out_shape=(
            jax.ShapeDtypeStruct((tall, 2 * width), BF16),
            jax.ShapeDtypeStruct((2, length, width), BF16),
            jax.ShapeDtypeStruct((2, length, width), F32),
        ),
        in_specs=vmem(3),
        out_specs=tuple(vmem(3)),
        name="local_maps",
    )(data, pal_data, forgetting_speed_exponent.T)
    joined, far = pl.pallas_call(
        combine_kernel,
        out_shape=(
            jax.ShapeDtypeStruct((tall, 2 * width), BF16),
            jax.ShapeDtypeStruct((tall, width), BF16),
        ),
        in_specs=vmem(2),
        out_specs=tuple(vmem(2)),
        name="combine_maps",
    )(message, passed(message, 1))
    mine, other = pl.pallas_call(
        apply_kernel,
        out_shape=(
            jax.ShapeDtypeStruct((length, width), F32),
            jax.ShapeDtypeStruct((length, width), BF16),
        ),
        in_specs=vmem(5),
        out_specs=tuple(vmem(2)),
        name="apply_state",
    )(message, passed(joined, 1), passed(far, 3), read, base)
    head_terms = pl.pallas_call(
        finish_kernel,
        out_shape=jax.ShapeDtypeStruct((8, length, blend_exit_weights.shape[1] // 8), BF16),
        in_specs=vmem(4),
        out_specs=vmem(1)[0],
        name="finish_mixer",
    )(mine, swapped(other), channel_group_scaling.reshape(1, width), blend_exit_weights)
    model_width = skip_path_inputs.shape[1]
    col_count = model_width // lax.axis_size("tp")
    col_start = lax.axis_index("tp") * col_count
    parts = lax.all_to_all(head_terms, "tp", 0, 0, tiled=True)
    own_residual = lax.dynamic_slice_in_dim(skip_path_inputs, col_start, col_count, 1).astype(
        F32
    ) + jnp.sum(parts.astype(F32), axis=0)
    sent_residual = own_residual.astype(BF16)
    both = jnp.concatenate([sent_residual, swapped(sent_residual)])
    residual = lax.all_gather(both, "tp", axis=1, tiled=True).astype(F32)
    squares = jnp.mean(residual * residual, axis=1, keepdims=True)
    normed = (residual * lax.rsqrt(squares + EPSILON) * dense_block_scaling).astype(BF16)
    raised = jnp.dot(normed, weights[:, :half], preferred_element_type=F32)
    active = jnp.square(jax.nn.relu(raised)).astype(BF16)
    lowered = lax.dot_general(active, weights[:, half:], NT, preferred_element_type=F32)
    turned = jnp.moveaxis(lowered.astype(BF16).reshape(2 * length, -1, col_count), 1, 0)
    pieces = lax.all_to_all(turned, "tp", 0, 0, tiled=True)
    sums = jnp.sum(pieces.astype(F32), axis=0)
    given = swapped(sums[length:].astype(BF16)).astype(F32)
    return (own_residual + sums[:length] + given).astype(BF16)


def solution(mesh):
    torus = Mesh(mesh.devices.reshape(8, 4, 2, mesh.shape["tp"]), (*SP, "tp"))
    placed = (
        P(SP, None),
        P(SP, "tp"),
        P(SP, "tp"),
        P(SP, "tp"),
        P(None, SP, "tp"),
        P(None, SP, "tp"),
        P(None, "tp"),
        P(None, SP, "tp"),
        P(SP),
        P(),
        P("tp", None),
        P(),
        P(SP, "tp"),
        P("tp", SP),
    )
    return jax.shard_map(
        shards, mesh=torus, in_specs=placed, out_specs=P(SP, "tp"), check_vma=False
    )
```

```python
import jax
import jax.numpy as jnp
from jax import lax
from jax.experimental import pallas as pl
from jax.experimental.pallas import tpu as pltpu
from jax.sharding import Mesh
from jax.sharding import PartitionSpec as P

SP = ("sp_0", "sp_1", "pair")
EPSILON = 1e-06
F32 = jnp.float32
BF16 = jnp.bfloat16
NT = (((1,), (1,)), ((), ()))
NN = (((1,), (0,)), ((), ()))


def mm(a, b, dims=NN):
    return lax.dot_general(a.astype(BF16), b.astype(BF16), dims, preferred_element_type=F32)


def split_in_two(a):
    high = a.astype(BF16)
    return high, (a - high.astype(F32)).astype(BF16)


def mm2(a, b, dims=NN):
    high, low = split_in_two(a)
    return mm(high, b, dims) + mm(low, b, dims)


def mm3(a, b):
    a_high, a_low = split_in_two(a)
    b_high, b_low = split_in_two(b)
    return mm(a_high, b_high) + (mm(a_high, b_low) + mm(a_low, b_high))


def pack_kernel(q_ref, k_ref, v_ref, strength_ref, forget_ref, spike_ref, docs_ref, out_ref):
    n, width = q_ref.shape
    for m, ref in enumerate((q_ref, k_ref, v_ref)):
        out_ref[:n, m * width : (m + 1) * width] = ref[...]
    docs = docs_ref[...].astype(F32)
    rest = jnp.concatenate([strength_ref[...], forget_ref[...], spike_ref[...], docs, docs])
    for m in range(3):
        piece = rest.astype(BF16)
        out_ref[n:, m * width : (m + 1) * width] = piece
        rest = rest - piece.astype(F32)


def local_kernel(own_ref, pal_ref, speed_ref, message_ref, read_ref, base_ref):
    n = own_ref.shape[0] - 8
    width = own_ref.shape[1] // 3
    back = lax.axis_index("pair")
    sign = 1 - 2 * back
    forward = back == 0
    rows = lax.broadcasted_iota(jnp.int32, (n, n), 0)
    cols = lax.broadcasted_iota(jnp.int32, (n, n), 1)
    eye = rows == cols
    reach = (rows - cols) * sign >= 0
    near = [((rows ^ cols) >> lg) == 1 for lg in range(7)]

    def to_col(row):
        return jnp.sum(jnp.where(eye, row, 0.0), axis=1, keepdims=True)

    def to_row(col):
        return jnp.sum(jnp.where(eye, col, 0.0), axis=0, keepdims=True)

    def chosen(pair):
        return jnp.where(forward, pair[0:1], pair[1:2])

    def block(data_ref):
        q, k, v = (data_ref[:n, m * width : (m + 1) * width] for m in range(3))
        high, middle, low = (
            data_ref[n:, m * width : (m + 1) * width].astype(F32) for m in range(3)
        )
        gates = (low + middle) + high
        beta_row = jax.nn.sigmoid(chosen(gates[0:2]))
        preacts = chosen(gates[2:4])
        soft = jnp.maximum(preacts, 0.0) + jnp.log1p(jnp.exp(-jnp.abs(preacts)))
        speed = jnp.where(forward, speed_ref[:, 0:1], speed_ref[:, 1:2])
        decay_row = -jnp.exp(speed) * soft + chosen(gates[4:6])
        docs_row = gates[6:7]
        docs_first = jnp.where(forward, docs_row[:, 0:1], docs_row[:, n - 1 : n])
        docs_last = jnp.where(forward, docs_row[:, n - 1 : n], docs_row[:, 0:1])
        docs_col = to_col(docs_row)
        qf, kf = q.astype(F32), k.astype(F32)
        q_scale = lax.rsqrt(jnp.sum(qf * qf, axis=1, keepdims=True) + EPSILON) * width ** (-0.5)
        k_scale = lax.rsqrt(jnp.sum(kf * kf, axis=1, keepdims=True) + EPSILON)
        k_scale_row = to_row(k_scale)
        similar = mm(k, k, NT) * k_scale * k_scale_row
        scored = mm(q, k, NT) * q_scale * k_scale_row
        running = jnp.sum(jnp.where(reach, decay_row, 0.0), axis=1, keepdims=True)
        running_row = to_row(running)
        total = jnp.sum(decay_row, axis=1, keepdims=True)
        within = reach & (docs_col == docs_row)
        spread = jnp.exp(jnp.where(within, running - running_row, -jnp.inf))
        strict = jnp.where(eye, 0.0, similar * spread * to_col(beta_row))
        inverse = jnp.where(eye, 1.0, 0.0) - jnp.where(near[0], strict, 0.0)
        for lg in range(1, 7):
            inverse = inverse - mm3(inverse, mm3(jnp.where(near[lg], strict, 0.0), inverse))
        linked_row = (docs_row == docs_first).astype(F32)
        linked = (docs_col == docs_first).astype(F32)
        ending_row = (docs_row == docs_last).astype(F32)
        update = mm2(inverse * beta_row, v)
        drop = mm2(inverse * (beta_row * jnp.exp(running_row) * linked_row * k_scale_row), k)
        tail = jnp.exp(jnp.minimum(total - running_row, 0.0))
        faded = jnp.transpose(kf) * (k_scale_row * tail * ending_row)
        kept = jnp.exp(total) * (docs_first == docs_last).astype(F32)
        step = jnp.where(eye, kept, 0.0) - mm(faded, drop)
        shift = mm(faded, update)
        scores = scored * spread
        read = qf * (q_scale * jnp.exp(running) * linked) - mm(scores, drop)
        return step, shift, read, mm(scores, update), docs_first, docs_last

    step, shift, read, base, docs_first, docs_mid = block(own_ref)
    pal_step, pal_shift, pal_read, pal_base, docs_next, docs_last = block(pal_ref)
    link = (docs_mid == docs_next).astype(F32)
    step, shift = step * link, shift * link
    message_ref[:n, :width] = mm(pal_step, step).astype(BF16)
    message_ref[:n, width:] = (mm(pal_step, shift) + pal_shift).astype(BF16)
    mark_docs(message_ref, n, docs_first, docs_last)
    read_ref[0] = read.astype(BF16)
    read_ref[1] = mm(pal_read, step).astype(BF16)
    base_ref[0] = base
    base_ref[1] = pal_base + mm(pal_read, shift)


def mark_docs(ref, n, docs_first, docs_last):
    ref[n : n + 8] = jnp.broadcast_to(docs_first, (8, ref.shape[1])).astype(BF16)
    ref[n + 8 :] = jnp.broadcast_to(docs_last, (8, ref.shape[1])).astype(BF16)


def combine_kernel(own_ref, in_ref, out_ref, far_ref):
    n = own_ref.shape[0] - 16
    docs_first = own_ref[n : n + 8, 0:1][0:1].astype(F32)
    in_last = in_ref[n + 8 :, 0:1][0:1].astype(F32)
    link = (docs_first == in_last).astype(F32)
    moved = mm(own_ref[:n, :n], in_ref[:n, :]) * link
    shift = (moved[:, n:] + own_ref[:n, n:].astype(F32)).astype(BF16)
    out_ref[:n, :n] = moved[:, :n].astype(BF16)
    out_ref[:n, n:] = shift
    out_ref[n : n + 8] = in_ref[n : n + 8]
    out_ref[n + 8 :] = own_ref[n + 8 :]
    far_ref[:n] = shift
    far_ref[n : n + 8] = in_ref[n : n + 8, :n]
    far_ref[n + 8 :] = own_ref[n + 8 :, :n]


def apply_kernel(own_ref, near_ref, far_ref, read_ref, base_ref, mine_ref, other_ref):
    n = own_ref.shape[0] - 16
    docs_first = own_ref[n : n + 8, 0:1][0:1].astype(F32)
    near_first = near_ref[n : n + 8, 0:1][0:1].astype(F32)
    near_last = near_ref[n + 8 :, 0:1][0:1].astype(F32)
    far_last = far_ref[n + 8 :, 0:1][0:1].astype(F32)
    state = mm(near_ref[:n, :n], far_ref[:n]) * (near_first == far_last).astype(F32)
    state = (state + near_ref[:n, n:].astype(F32)) * (docs_first == near_last).astype(F32)
    other_ref[...] = (base_ref[1] + mm(read_ref[1], state)).astype(BF16)
    mine_ref[...] = base_ref[0] + mm(read_ref[0], state)


def finish_kernel(mine_ref, in_ref, gain_ref, exit_ref, out_ref):
    attn = mine_ref[...] + in_ref[...].astype(F32)
    mean = jnp.mean(attn * attn, axis=1, keepdims=True)
    mixed = (attn * lax.rsqrt(mean + EPSILON) * gain_ref[...]).astype(BF16)
    terms = mm(mixed, exit_ref[...]).astype(BF16)
    step = out_ref.shape[2]
    for m in range(out_ref.shape[0]):
        out_ref[m] = terms[:, m * step : (m + 1) * step]


def vmem(count):
    return [pl.BlockSpec(memory_space=pltpu.VMEM)] * count


def shards(
    skip_path_inputs,
    probe_vectors,
    lookup_vectors,
    payload_vectors,
    learning_strength_preacts,
    forget_preacts,
    forgetting_speed_exponent,
    extra_forgetting_spikes,
    sample_membership,
    channel_group_scaling,
    blend_exit_weights,
    dense_block_scaling,
    widen_projection_weights,
    shrink_projection_weights,
):
    length, width = probe_vectors.shape
    count = lax.axis_size(SP)

    def swapped(array):
        return lax.ppermute(array, SP, [(i, i ^ 1) for i in range(count)])

    def passed(array, distance):
        ways = (2 * distance, -2 * distance)
        return lax.ppermute(array, SP, [(i, (i + ways[i % 2]) % count) for i in range(count)])

    data = pl.pallas_call(
        pack_kernel,
        out_shape=jax.ShapeDtypeStruct((length + 8, 3 * width), BF16),
        in_specs=vmem(7),
        out_specs=vmem(1)[0],
        name="pack_inputs",
    )(
        probe_vectors,
        lookup_vectors,
        payload_vectors,
        learning_strength_preacts.reshape(2, length),
        forget_preacts.reshape(2, length),
        extra_forgetting_spikes.reshape(2, length),
        sample_membership.reshape(1, length),
    )
    pal_data = swapped(data)
    up_width = widen_projection_weights.shape[1]
    weights = lax.all_gather(
        jnp.concatenate([widen_projection_weights, shrink_projection_weights.T], axis=1),
        SP,
        axis=0,
        tiled=True,
    )
    tall = width + 16
    message, read, base = pl.pallas_call(
        local_kernel,
        out_shape=(
            jax.ShapeDtypeStruct((tall, 2 * width), BF16),
            jax.ShapeDtypeStruct((2, length, width), BF16),
            jax.ShapeDtypeStruct((2, length, width), F32),
        ),
        in_specs=vmem(3),
        out_specs=tuple(vmem(3)),
        name="local_maps",
    )(data, pal_data, forgetting_speed_exponent.T)
    joined, far = pl.pallas_call(
        combine_kernel,
        out_shape=(
            jax.ShapeDtypeStruct((tall, 2 * width), BF16),
            jax.ShapeDtypeStruct((tall, width), BF16),
        ),
        in_specs=vmem(2),
        out_specs=tuple(vmem(2)),
        name="combine_maps",
    )(message, passed(message, 1))
    mine, other = pl.pallas_call(
        apply_kernel,
        out_shape=(
            jax.ShapeDtypeStruct((length, width), F32),
            jax.ShapeDtypeStruct((length, width), BF16),
        ),
        in_specs=vmem(5),
        out_specs=tuple(vmem(2)),
        name="apply_state",
    )(message, passed(joined, 1), passed(far, 3), read, base)
    head_terms = pl.pallas_call(
        finish_kernel,
        out_shape=jax.ShapeDtypeStruct((8, length, blend_exit_weights.shape[1] // 8), BF16),
        in_specs=vmem(4),
        out_specs=vmem(1)[0],
        name="finish_mixer",
    )(mine, swapped(other), channel_group_scaling.reshape(1, width), blend_exit_weights)
    model_width = skip_path_inputs.shape[1]
    col_count = model_width // lax.axis_size("tp")
    col_start = lax.axis_index("tp") * col_count
    parts = lax.all_to_all(head_terms, "tp", 0, 0, tiled=True)
    own_residual = lax.dynamic_slice_in_dim(skip_path_inputs, col_start, col_count, 1).astype(
        F32
    ) + jnp.sum(parts.astype(F32), axis=0)
    residual = lax.all_gather(own_residual.astype(BF16), "tp", axis=1, tiled=True).astype(F32)
    squares = jnp.mean(residual * residual, axis=1, keepdims=True)
    normed = (residual * lax.rsqrt(squares + EPSILON) * dense_block_scaling).astype(BF16)
    raised = jnp.dot(normed, weights[:, :up_width], preferred_element_type=F32)
    active = jnp.square(jax.nn.relu(raised)).astype(BF16)
    lowered = lax.dot_general(active, weights[:, up_width:], NT, preferred_element_type=F32)
    turned = jnp.moveaxis(lowered.astype(BF16).reshape(length, -1, col_count), 1, 0)
    pieces = lax.all_to_all(turned, "tp", 0, 0, tiled=True)
    return (own_residual + jnp.sum(pieces.astype(F32), axis=0)).astype(BF16)


def solution(mesh):
    torus = Mesh(mesh.devices.reshape(8, 4, 2, mesh.shape["tp"]), (*SP, "tp"))
    placed = (
        P(SP, None),
        P(SP, "tp"),
        P(SP, "tp"),
        P(SP, "tp"),
        P(None, SP, "tp"),
        P(None, SP, "tp"),
        P(None, "tp"),
        P(None, SP, "tp"),
        P(SP),
        P(),
        P("tp", None),
        P(),
        P(SP, "tp"),
        P("tp", SP),
    )
    return jax.shard_map(
        shards, mesh=torus, in_specs=placed, out_specs=P(SP, "tp"), check_vma=False
    )
```

```python
import jax
import jax.numpy as jnp
from jax import lax
from jax.experimental import pallas as pl
from jax.experimental.pallas import tpu as pltpu
from jax.sharding import Mesh
from jax.sharding import PartitionSpec as P

SP = ("sp_0", "sp_1", "pair")
EPSILON = 1e-06
F32 = jnp.float32
BF16 = jnp.bfloat16
NT = (((1,), (1,)), ((), ()))
NN = (((1,), (0,)), ((), ()))


def mm(a, b, dims=NN):
    return lax.dot_general(a.astype(BF16), b.astype(BF16), dims, preferred_element_type=F32)


def split_in_two(a):
    high = a.astype(BF16)
    return high, (a - high.astype(F32)).astype(BF16)


def mm2(a, b, dims=NN):
    high, low = split_in_two(a)
    return mm(high, b, dims) + mm(low, b, dims)


def mm3(a, b):
    a_high, a_low = split_in_two(a)
    b_high, b_low = split_in_two(b)
    return mm(a_high, b_high) + (mm(a_high, b_low) + mm(a_low, b_high))


def pack_kernel(q_ref, k_ref, v_ref, strength_ref, forget_ref, spike_ref, docs_ref, out_ref):
    n, width = q_ref.shape
    for m, ref in enumerate((q_ref, k_ref, v_ref)):
        out_ref[:n, m * width : (m + 1) * width] = ref[...]
    docs = docs_ref[...].astype(F32)
    rest = jnp.concatenate([strength_ref[...], forget_ref[...], spike_ref[...], docs, docs])
    for m in range(3):
        piece = rest.astype(BF16)
        out_ref[n:, m * width : (m + 1) * width] = piece
        rest = rest - piece.astype(F32)


def local_kernel(own_ref, pal_ref, speed_ref, message_ref, read_ref, base_ref):
    n = own_ref.shape[0] - 8
    width = own_ref.shape[1] // 3
    back = lax.axis_index("pair")
    sign = 1 - 2 * back
    forward = back == 0
    rows = lax.broadcasted_iota(jnp.int32, (n, n), 0)
    cols = lax.broadcasted_iota(jnp.int32, (n, n), 1)
    eye = rows == cols
    reach = (rows - cols) * sign >= 0
    near = [((rows ^ cols) >> lg) == 1 for lg in range(7)]

    def to_col(row):
        return jnp.sum(jnp.where(eye, row, 0.0), axis=1, keepdims=True)

    def to_row(col):
        return jnp.sum(jnp.where(eye, col, 0.0), axis=0, keepdims=True)

    def chosen(pair):
        return jnp.where(forward, pair[0:1], pair[1:2])

    def block(data_ref):
        q, k, v = (data_ref[:n, m * width : (m + 1) * width] for m in range(3))
        high, middle, low = (
            data_ref[n:, m * width : (m + 1) * width].astype(F32) for m in range(3)
        )
        gates = (low + middle) + high
        beta_row = jax.nn.sigmoid(chosen(gates[0:2]))
        preacts = chosen(gates[2:4])
        soft = jnp.maximum(preacts, 0.0) + jnp.log1p(jnp.exp(-jnp.abs(preacts)))
        speed = jnp.where(forward, speed_ref[:, 0:1], speed_ref[:, 1:2])
        decay_row = -jnp.exp(speed) * soft + chosen(gates[4:6])
        docs_row = gates[6:7]
        docs_first = jnp.where(forward, docs_row[:, 0:1], docs_row[:, n - 1 : n])
        docs_last = jnp.where(forward, docs_row[:, n - 1 : n], docs_row[:, 0:1])
        docs_col = to_col(docs_row)
        qf, kf = q.astype(F32), k.astype(F32)
        q_scale = lax.rsqrt(jnp.sum(qf * qf, axis=1, keepdims=True) + EPSILON) * width ** (-0.5)
        k_scale = lax.rsqrt(jnp.sum(kf * kf, axis=1, keepdims=True) + EPSILON)
        k_scale_row = to_row(k_scale)
        similar = mm(k, k, NT) * k_scale * k_scale_row
        scored = mm(q, k, NT) * q_scale * k_scale_row
        running = jnp.sum(jnp.where(reach, decay_row, 0.0), axis=1, keepdims=True)
        running_row = to_row(running)
        total = jnp.sum(decay_row, axis=1, keepdims=True)
        within = reach & (docs_col == docs_row)
        spread = jnp.exp(jnp.where(within, running - running_row, -jnp.inf))
        strict = jnp.where(eye, 0.0, similar * spread * to_col(beta_row))
        inverse = jnp.where(eye, 1.0, 0.0) - jnp.where(near[0], strict, 0.0)
        for lg in range(1, 7):
            inverse = inverse - mm3(inverse, mm3(jnp.where(near[lg], strict, 0.0), inverse))
        linked_row = (docs_row == docs_first).astype(F32)
        linked = (docs_col == docs_first).astype(F32)
        ending_row = (docs_row == docs_last).astype(F32)
        update = mm2(inverse * beta_row, v)
        drop = mm2(inverse * (beta_row * jnp.exp(running_row) * linked_row * k_scale_row), k)
        tail = jnp.exp(jnp.minimum(total - running_row, 0.0))
        faded = jnp.transpose(kf) * (k_scale_row * tail * ending_row)
        kept = jnp.exp(total) * (docs_first == docs_last).astype(F32)
        step = jnp.where(eye, kept, 0.0) - mm3(faded, drop)
        shift = mm3(faded, update)
        scores = scored * spread
        read = qf * (q_scale * jnp.exp(running) * linked) - mm3(scores, drop)
        return step, shift, read, mm3(scores, update), docs_first, docs_last

    step, shift, read, base, docs_first, docs_mid = block(own_ref)
    pal_step, pal_shift, pal_read, pal_base, docs_next, docs_last = block(pal_ref)
    link = (docs_mid == docs_next).astype(F32)
    step, shift = step * link, shift * link
    message_ref[:n, :width] = mm(pal_step, step).astype(BF16)
    message_ref[:n, width:] = (mm(pal_step, shift) + pal_shift).astype(BF16)
    mark_docs(message_ref, n, docs_first, docs_last)
    read_ref[0] = read.astype(BF16)
    read_ref[1] = mm(pal_read, step).astype(BF16)
    base_ref[0] = base
    base_ref[1] = pal_base + mm(pal_read, shift)


def mark_docs(ref, n, docs_first, docs_last):
    ref[n : n + 8] = jnp.broadcast_to(docs_first, (8, ref.shape[1])).astype(BF16)
    ref[n + 8 :] = jnp.broadcast_to(docs_last, (8, ref.shape[1])).astype(BF16)


def combine_kernel(own_ref, in_ref, out_ref, far_ref):
    n = own_ref.shape[0] - 16
    docs_first = own_ref[n : n + 8, 0:1][0:1].astype(F32)
    in_last = in_ref[n + 8 :, 0:1][0:1].astype(F32)
    link = (docs_first == in_last).astype(F32)
    moved = mm(own_ref[:n, :n], in_ref[:n, :]) * link
    shift = (moved[:, n:] + own_ref[:n, n:].astype(F32)).astype(BF16)
    out_ref[:n, :n] = moved[:, :n].astype(BF16)
    out_ref[:n, n:] = shift
    out_ref[n : n + 8] = in_ref[n : n + 8]
    out_ref[n + 8 :] = own_ref[n + 8 :]
    far_ref[:n] = shift
    far_ref[n : n + 8] = in_ref[n : n + 8, :n]
    far_ref[n + 8 :] = own_ref[n + 8 :, :n]


def apply_kernel(own_ref, near_ref, far_ref, read_ref, base_ref, mine_ref, other_ref):
    n = own_ref.shape[0] - 16
    docs_first = own_ref[n : n + 8, 0:1][0:1].astype(F32)
    near_first = near_ref[n : n + 8, 0:1][0:1].astype(F32)
    near_last = near_ref[n + 8 :, 0:1][0:1].astype(F32)
    far_last = far_ref[n + 8 :, 0:1][0:1].astype(F32)
    state = mm(near_ref[:n, :n], far_ref[:n]) * (near_first == far_last).astype(F32)
    state = (state + near_ref[:n, n:].astype(F32)) * (docs_first == near_last).astype(F32)
    other_ref[...] = (base_ref[1] + mm(read_ref[1], state)).astype(BF16)
    mine_ref[...] = base_ref[0] + mm(read_ref[0], state)


def finish_kernel(mine_ref, in_ref, gain_ref, exit_ref, out_ref):
    attn = mine_ref[...] + in_ref[...].astype(F32)
    mean = jnp.mean(attn * attn, axis=1, keepdims=True)
    mixed = (attn * lax.rsqrt(mean + EPSILON) * gain_ref[...]).astype(BF16)
    terms = mm(mixed, exit_ref[...]).astype(BF16)
    step = out_ref.shape[2]
    for m in range(out_ref.shape[0]):
        out_ref[m] = terms[:, m * step : (m + 1) * step]


def vmem(count):
    return [pl.BlockSpec(memory_space=pltpu.VMEM)] * count


def shards(
    skip_path_inputs,
    probe_vectors,
    lookup_vectors,
    payload_vectors,
    learning_strength_preacts,
    forget_preacts,
    forgetting_speed_exponent,
    extra_forgetting_spikes,
    sample_membership,
    channel_group_scaling,
    blend_exit_weights,
    dense_block_scaling,
    widen_projection_weights,
    shrink_projection_weights,
):
    length, width = probe_vectors.shape
    count = lax.axis_size(SP)

    def swapped(array):
        return lax.ppermute(array, SP, [(i, i ^ 1) for i in range(count)])

    def passed(array, distance):
        ways = (2 * distance, -2 * distance)
        return lax.ppermute(array, SP, [(i, (i + ways[i % 2]) % count) for i in range(count)])

    data = pl.pallas_call(
        pack_kernel,
        out_shape=jax.ShapeDtypeStruct((length + 8, 3 * width), BF16),
        in_specs=vmem(7),
        out_specs=vmem(1)[0],
        name="pack_inputs",
    )(
        probe_vectors,
        lookup_vectors,
        payload_vectors,
        learning_strength_preacts.reshape(2, length),
        forget_preacts.reshape(2, length),
        extra_forgetting_spikes.reshape(2, length),
        sample_membership.reshape(1, length),
    )
    pal_data = swapped(data)
    up_width = widen_projection_weights.shape[1]
    weights = lax.all_gather(
        jnp.concatenate([widen_projection_weights, shrink_projection_weights.T], axis=1),
        SP,
        axis=0,
        tiled=True,
    )
    tall = width + 16
    message, read, base = pl.pallas_call(
        local_kernel,
        out_shape=(
            jax.ShapeDtypeStruct((tall, 2 * width), BF16),
            jax.ShapeDtypeStruct((2, length, width), BF16),
            jax.ShapeDtypeStruct((2, length, width), F32),
        ),
        in_specs=vmem(3),
        out_specs=tuple(vmem(3)),
        name="local_maps",
    )(data, pal_data, forgetting_speed_exponent.T)
    joined, far = pl.pallas_call(
        combine_kernel,
        out_shape=(
            jax.ShapeDtypeStruct((tall, 2 * width), BF16),
            jax.ShapeDtypeStruct((tall, width), BF16),
        ),
        in_specs=vmem(2),
        out_specs=tuple(vmem(2)),
        name="combine_maps",
    )(message, passed(message, 1))
    mine, other = pl.pallas_call(
        apply_kernel,
        out_shape=(
            jax.ShapeDtypeStruct((length, width), F32),
            jax.ShapeDtypeStruct((length, width), BF16),
        ),
        in_specs=vmem(5),
        out_specs=tuple(vmem(2)),
        name="apply_state",
    )(message, passed(joined, 1), passed(far, 3), read, base)
    head_terms = pl.pallas_call(
        finish_kernel,
        out_shape=jax.ShapeDtypeStruct((8, length, blend_exit_weights.shape[1] // 8), BF16),
        in_specs=vmem(4),
        out_specs=vmem(1)[0],
        name="finish_mixer",
    )(mine, swapped(other), channel_group_scaling.reshape(1, width), blend_exit_weights)
    model_width = skip_path_inputs.shape[1]
    col_count = model_width // lax.axis_size("tp")
    col_start = lax.axis_index("tp") * col_count
    parts = lax.all_to_all(head_terms, "tp", 0, 0, tiled=True)
    own_residual = lax.dynamic_slice_in_dim(skip_path_inputs, col_start, col_count, 1).astype(
        F32
    ) + jnp.sum(parts.astype(F32), axis=0)
    residual = lax.all_gather(own_residual.astype(BF16), "tp", axis=1, tiled=True).astype(F32)
    squares = jnp.mean(residual * residual, axis=1, keepdims=True)
    normed = (residual * lax.rsqrt(squares + EPSILON) * dense_block_scaling).astype(BF16)
    raised = jnp.dot(normed, weights[:, :up_width], preferred_element_type=F32)
    active = jnp.square(jax.nn.relu(raised)).astype(BF16)
    lowered = lax.dot_general(active, weights[:, up_width:], NT, preferred_element_type=F32)
    turned = jnp.moveaxis(lowered.astype(BF16).reshape(length, -1, col_count), 1, 0)
    pieces = lax.all_to_all(turned, "tp", 0, 0, tiled=True)
    return (own_residual + jnp.sum(pieces.astype(F32), axis=0)).astype(BF16)


def solution(mesh):
    torus = Mesh(mesh.devices.reshape(8, 4, 2, mesh.shape["tp"]), (*SP, "tp"))
    placed = (
        P(SP, None),
        P(SP, "tp"),
        P(SP, "tp"),
        P(SP, "tp"),
        P(None, SP, "tp"),
        P(None, SP, "tp"),
        P(None, "tp"),
        P(None, SP, "tp"),
        P(SP),
        P(),
        P("tp", None),
        P(),
        P(SP, "tp"),
        P("tp", SP),
    )
    return jax.shard_map(
        shards, mesh=torus, in_specs=placed, out_specs=P(SP, "tp"), check_vma=False
    )
```

```python
import jax
import jax.numpy as jnp
from jax import lax
from jax.experimental import pallas as pl
from jax.experimental.pallas import tpu as pltpu
from jax.sharding import Mesh
from jax.sharding import PartitionSpec as P

SP = ("sp_0", "sp_1", "pair")
EPSILON = 1e-06
SIDE = 128
F32 = jnp.float32
BF16 = jnp.bfloat16
NT = (((1,), (1,)), ((), ()))
NN = (((1,), (0,)), ((), ()))


def mm(a, b, dims=NN):
    return lax.dot_general(a.astype(BF16), b.astype(BF16), dims, preferred_element_type=F32)


def split_in_two(a):
    high = a.astype(BF16)
    return high, (a - high.astype(F32)).astype(BF16)


def mm2(a, b, dims=NN):
    high, low = split_in_two(a)
    return mm(high, b, dims) + mm(low, b, dims)


def mm3(a, b):
    a_high, a_low = split_in_two(a)
    b_high, b_low = split_in_two(b)
    return mm(a_high, b_high) + (mm(a_high, b_low) + mm(a_low, b_high))


def pack_kernel(q_ref, k_ref, v_ref, strength_ref, forget_ref, spike_ref, docs_ref, out_ref):
    n, width = q_ref.shape
    for m, ref in enumerate((q_ref, k_ref, v_ref)):
        out_ref[:n, m * width : (m + 1) * width] = ref[...]
    docs = docs_ref[...].astype(F32)
    rest = jnp.concatenate([strength_ref[...], forget_ref[...], spike_ref[...], docs, docs])
    for m in range(3):
        piece = rest.astype(BF16)
        out_ref[n:, m * width : (m + 1) * width] = piece
        rest = rest - piece.astype(F32)


def local_kernel(own_ref, pal_ref, speed_ref, message_ref, read_ref, base_ref):
    n = own_ref.shape[0] - 8
    width = own_ref.shape[1] // 3
    back = lax.axis_index("pair")
    sign = 1 - 2 * back
    forward = back == 0
    rows = lax.broadcasted_iota(jnp.int32, (n, n), 0)
    cols = lax.broadcasted_iota(jnp.int32, (n, n), 1)
    eye = rows == cols
    reach = (rows - cols) * sign >= 0
    near = [((rows ^ cols) >> lg) == 1 for lg in range(7)]

    def to_col(row):
        return jnp.sum(jnp.where(eye, row, 0.0), axis=1, keepdims=True)

    def to_row(col):
        return jnp.sum(jnp.where(eye, col, 0.0), axis=0, keepdims=True)

    def chosen(pair):
        return jnp.where(forward, pair[0:1], pair[1:2])

    def block(data_ref):
        q, k, v = (data_ref[:n, m * width : (m + 1) * width] for m in range(3))
        high, middle, low = (
            data_ref[n:, m * width : (m + 1) * width].astype(F32) for m in range(3)
        )
        gates = (low + middle) + high
        beta_row = jax.nn.sigmoid(chosen(gates[0:2]))
        preacts = chosen(gates[2:4])
        soft = jnp.maximum(preacts, 0.0) + jnp.log1p(jnp.exp(-jnp.abs(preacts)))
        speed = jnp.where(forward, speed_ref[:, 0:1], speed_ref[:, 1:2])
        decay_row = -jnp.exp(speed) * soft + chosen(gates[4:6])
        docs_row = gates[6:7]
        docs_first = jnp.where(forward, docs_row[:, 0:1], docs_row[:, n - 1 : n])
        docs_last = jnp.where(forward, docs_row[:, n - 1 : n], docs_row[:, 0:1])
        docs_col = to_col(docs_row)
        qf, kf = q.astype(F32), k.astype(F32)
        q_scale = lax.rsqrt(jnp.sum(qf * qf, axis=1, keepdims=True) + EPSILON) * width ** (-0.5)
        k_scale = lax.rsqrt(jnp.sum(kf * kf, axis=1, keepdims=True) + EPSILON)
        k_scale_row = to_row(k_scale)
        similar = mm(k, k, NT) * k_scale * k_scale_row
        scored = mm(q, k, NT) * q_scale * k_scale_row
        running = jnp.sum(jnp.where(reach, decay_row, 0.0), axis=1, keepdims=True)
        running_row = to_row(running)
        total = jnp.sum(decay_row, axis=1, keepdims=True)
        within = reach & (docs_col == docs_row)
        spread = jnp.exp(jnp.where(within, running - running_row, -jnp.inf))
        strict = jnp.where(eye, 0.0, similar * spread * to_col(beta_row))
        inverse = jnp.where(eye, 1.0, 0.0) - jnp.where(near[0], strict, 0.0)
        for lg in range(1, 7):
            inverse = inverse - mm3(inverse, mm3(jnp.where(near[lg], strict, 0.0), inverse))
        linked_row = (docs_row == docs_first).astype(F32)
        linked = (docs_col == docs_first).astype(F32)
        ending_row = (docs_row == docs_last).astype(F32)
        update = mm2(inverse * beta_row, v)
        drop = mm2(inverse * (beta_row * jnp.exp(running_row) * linked_row * k_scale_row), k)
        tail = jnp.exp(jnp.minimum(total - running_row, 0.0))
        faded = jnp.transpose(kf) * (k_scale_row * tail * ending_row)
        kept = jnp.exp(total) * (docs_first == docs_last).astype(F32)
        step = jnp.where(eye, kept, 0.0) - mm3(faded, drop)
        shift = mm3(faded, update)
        scores = scored * spread
        read = qf * (q_scale * jnp.exp(running) * linked) - mm3(scores, drop)
        return step, shift, read, mm3(scores, update), docs_first, docs_last

    step, shift, read, base, docs_first, docs_mid = block(own_ref)
    pal_step, pal_shift, pal_read, pal_base, docs_next, docs_last = block(pal_ref)
    link = (docs_mid == docs_next).astype(F32)
    step, shift = step * link, shift * link
    message_ref[:n, :width] = mm(pal_step, step).astype(BF16)
    message_ref[:n, width:] = (mm(pal_step, shift) + pal_shift).astype(BF16)
    mark_docs(message_ref, n, docs_first, docs_last)
    read_ref[0] = read.astype(BF16)
    read_ref[1] = mm(pal_read, step).astype(BF16)
    base_ref[0] = base
    base_ref[1] = pal_base + mm(pal_read, shift)


def mark_docs(ref, n, docs_first, docs_last):
    ref[n : n + 8] = jnp.broadcast_to(docs_first, (8, ref.shape[1])).astype(BF16)
    ref[n + 8 :] = jnp.broadcast_to(docs_last, (8, ref.shape[1])).astype(BF16)


def combine_kernel(own_ref, in_ref, out_ref, far_ref):
    n = own_ref.shape[0] - 16
    docs_first = own_ref[n : n + 8, 0:1][0:1].astype(F32)
    in_last = in_ref[n + 8 :, 0:1][0:1].astype(F32)
    link = (docs_first == in_last).astype(F32)
    moved = mm(own_ref[:n, :n], in_ref[:n, :]) * link
    shift = (moved[:, n:] + own_ref[:n, n:].astype(F32)).astype(BF16)
    out_ref[:n, :n] = moved[:, :n].astype(BF16)
    out_ref[:n, n:] = shift
    out_ref[n : n + 8] = in_ref[n : n + 8]
    out_ref[n + 8 :] = own_ref[n + 8 :]
    far_ref[:n] = shift
    far_ref[n : n + 8] = in_ref[n : n + 8, :n]
    far_ref[n + 8 :] = own_ref[n + 8 :, :n]


def apply_kernel(own_ref, near_ref, far_ref, read_ref, base_ref, mine_ref, other_ref):
    n = own_ref.shape[0] - 16
    docs_first = own_ref[n : n + 8, 0:1][0:1].astype(F32)
    near_first = near_ref[n : n + 8, 0:1][0:1].astype(F32)
    near_last = near_ref[n + 8 :, 0:1][0:1].astype(F32)
    far_last = far_ref[n + 8 :, 0:1][0:1].astype(F32)
    state = mm(near_ref[:n, :n], far_ref[:n]) * (near_first == far_last).astype(F32)
    state = (state + near_ref[:n, n:].astype(F32)) * (docs_first == near_last).astype(F32)
    other_ref[...] = (base_ref[1] + mm(read_ref[1], state)).astype(BF16)
    mine_ref[...] = base_ref[0] + mm(read_ref[0], state)


def finish_kernel(mine_ref, in_ref, gain_ref, exit_ref, out_ref):
    attn = mine_ref[...] + in_ref[...].astype(F32)
    mean = jnp.mean(attn * attn, axis=1, keepdims=True)
    mixed = (attn * lax.rsqrt(mean + EPSILON) * gain_ref[...]).astype(BF16)
    terms = mm(mixed, exit_ref[...]).astype(BF16)
    step = out_ref.shape[2]
    for m in range(out_ref.shape[0]):
        out_ref[m] = terms[:, m * step : (m + 1) * step]


def vmem(count):
    return [pl.BlockSpec(memory_space=pltpu.VMEM)] * count


def shards(
    skip_path_inputs,
    probe_vectors,
    lookup_vectors,
    payload_vectors,
    learning_strength_preacts,
    forget_preacts,
    forgetting_speed_exponent,
    extra_forgetting_spikes,
    sample_membership,
    channel_group_scaling,
    blend_exit_weights,
    dense_block_scaling,
    widen_projection_weights,
    shrink_projection_weights,
):
    length, width = probe_vectors.shape
    count = lax.axis_size(SP)

    def swapped(array):
        return lax.ppermute(array, SP, [(i, i ^ 1) for i in range(count)])

    def passed(array, distance):
        ways = (2 * distance, -2 * distance)
        return lax.ppermute(array, SP, [(i, (i + ways[i % 2]) % count) for i in range(count)])

    data = pl.pallas_call(
        pack_kernel,
        out_shape=jax.ShapeDtypeStruct((length + 8, 3 * width), BF16),
        in_specs=vmem(7),
        out_specs=vmem(1)[0],
        name="pack_inputs",
    )(
        probe_vectors,
        lookup_vectors,
        payload_vectors,
        learning_strength_preacts.reshape(2, length),
        forget_preacts.reshape(2, length),
        extra_forgetting_spikes.reshape(2, length),
        sample_membership.reshape(1, length),
    )
    pal_data = swapped(data)
    up_width = widen_projection_weights.shape[1] - SIDE
    turned_down = shrink_projection_weights.T
    weights = lax.all_gather(
        jnp.concatenate([widen_projection_weights[:, :up_width], turned_down[:, :up_width]], axis=1),
        SP,
        axis=0,
        tiled=True,
    )
    few = jnp.concatenate([widen_projection_weights[:, up_width:], turned_down[:, up_width:]], axis=1)
    for axes in (SP[1:], SP[:1]):
        size = lax.axis_size(axes)
        copies = jnp.broadcast_to(few[None], (size, *few.shape))
        few = lax.all_to_all(copies, axes, 0, 0, tiled=True).reshape(-1, few.shape[1])
    tall = width + 16
    message, read, base = pl.pallas_call(
        local_kernel,
        out_shape=(
            jax.ShapeDtypeStruct((tall, 2 * width), BF16),
            jax.ShapeDtypeStruct((2, length, width), BF16),
            jax.ShapeDtypeStruct((2, length, width), F32),
        ),
        in_specs=vmem(3),
        out_specs=tuple(vmem(3)),
        name="local_maps",
    )(data, pal_data, forgetting_speed_exponent.T)
    before = passed(message, 1)
    joined, far = pl.pallas_call(
        combine_kernel,
        out_shape=(
            jax.ShapeDtypeStruct((tall, 2 * width), BF16),
            jax.ShapeDtypeStruct((tall, width), BF16),
        ),
        in_specs=vmem(2),
        out_specs=tuple(vmem(2)),
        name="combine_maps",
    )(message, before)
    mine, other = pl.pallas_call(
        apply_kernel,
        out_shape=(
            jax.ShapeDtypeStruct((length, width), F32),
            jax.ShapeDtypeStruct((length, width), BF16),
        ),
        in_specs=vmem(5),
        out_specs=tuple(vmem(2)),
        name="apply_state",
    )(message, passed(joined, 1), passed(far, 3), read, base)
    head_terms = pl.pallas_call(
        finish_kernel,
        out_shape=jax.ShapeDtypeStruct((8, length, blend_exit_weights.shape[1] // 8), BF16),
        in_specs=vmem(4),
        out_specs=vmem(1)[0],
        name="finish_mixer",
    )(mine, swapped(other), channel_group_scaling.reshape(1, width), blend_exit_weights)
    few, head_terms = lax.optimization_barrier((few, head_terms))
    model_width = skip_path_inputs.shape[1]
    col_count = model_width // lax.axis_size("tp")
    col_start = lax.axis_index("tp") * col_count
    parts = lax.all_to_all(head_terms, "tp", 0, 0, tiled=True)
    own_residual = lax.dynamic_slice_in_dim(skip_path_inputs, col_start, col_count, 1).astype(
        F32
    ) + jnp.sum(parts.astype(F32), axis=0)
    residual = lax.all_gather(own_residual.astype(BF16), "tp", axis=1, tiled=True).astype(F32)
    squares = jnp.mean(residual * residual, axis=1, keepdims=True)
    normed = (residual * lax.rsqrt(squares + EPSILON) * dense_block_scaling).astype(BF16)

    def fed(matrix, middle):
        raised = jnp.dot(normed, matrix[:, :middle], preferred_element_type=F32)
        active = jnp.square(jax.nn.relu(raised)).astype(BF16)
        return lax.dot_general(active, matrix[:, middle:], NT, preferred_element_type=F32)

    lowered = fed(few, SIDE) + fed(weights, up_width)
    turned = jnp.moveaxis(lowered.astype(BF16).reshape(length, -1, col_count), 1, 0)
    pieces = lax.all_to_all(turned, "tp", 0, 0, tiled=True)
    return (own_residual + jnp.sum(pieces.astype(F32), axis=0)).astype(BF16)


def solution(mesh):
    torus = Mesh(mesh.devices.reshape(8, 4, 2, mesh.shape["tp"]), (*SP, "tp"))
    placed = (
        P(SP, None),
        P(SP, "tp"),
        P(SP, "tp"),
        P(SP, "tp"),
        P(None, SP, "tp"),
        P(None, SP, "tp"),
        P(None, "tp"),
        P(None, SP, "tp"),
        P(SP),
        P(),
        P("tp", None),
        P(),
        P(SP, "tp"),
        P("tp", SP),
    )

    return jax.shard_map(
        shards, mesh=torus, in_specs=placed, out_specs=P(SP, "tp"), check_vma=False
    )
```
